32 devices in a mesh: rep: 2 (over core), fs: 8 (over z, y), tp: 2 (over x).
Axes of the slice: x: 2, y: 2, z: 4, core: 2. Of those that a mesh axis runs over, the one named last changes fastest.
Arguments:
- resid: bfloat16 [16, 1024, 2048], P(('rep', 'fs')), may hold values from -6 to 6
- attention_norm_gain: float32 [2048], replicated, may hold values from 0.1 to 1.9
- query_weight: bfloat16 [2048, 1024], P('fs', 'tp'), may hold values from -0.125 to 0.125
- key_weight: bfloat16 [2048, 1024], P('fs', 'tp'), may hold values from -0.125 to 0.125
- value_weight: bfloat16 [2048, 2048], P('fs', 'tp'), may hold values from -0.125 to 0.125
- decay_down_weight: bfloat16 [2048, 16], replicated, may hold values from -0.125 to 0.125
- decay_up_weight: bfloat16 [16, 1024], replicated, may hold values from -1.5 to 1.5
- decay_rate_bias: float32 [1024], replicated, may hold values from 0.3 to 7
- decay_increment: float32 [16, 1024, 8], P(('rep', 'fs'), None, 'tp'), may hold values from -0.7 to 0, as said below
- head_norm_gain: float32 [256], replicated, may hold values from 0.1 to 1.9
- feedforward_norm_gain: float32 [2048], replicated, may hold values from 0.1 to 1.9
- up_weight: bfloat16 [2048, 4096], P('fs', 'tp'), may hold values from -0.125 to 0.125
- down_weight: bfloat16 [4096, 2048], P('tp', 'fs'), may hold values from -0.09375 to 0.09375
Outputs:
- layer_out: bfloat16 [16, 1024, 2048], P(('rep', 'fs'), None, 'tp')
The draws below stay inside these ranges and needn't reach their ends.
Inputs may be any that keep to these rules, and one draw needn't show every extreme that they name: `decay_increment`: each entry is zero or a negative log-decay.
All inputs are finite; a program needn't handle non-finite values.
Results may differ from the reference program's by a relative error of at most 0.014.
Values may be sent and summed in bfloat16 or wider, within the bound.
A program may use at most 64 MiB of HBM per device.

```python
import jax
import jax.numpy as jnp
from jax import lax

D = 2048
ATTENTION_HEADS = 8
KEY_CHANNELS = 128
HEAD_V = 256
RANK = 16
FF = 4096
BLOCK = 64
LEN = 1024
SEQS = 16
N_TP = 2


def draw_decay_rate_bias(key, part):
    head_key, chan_key = jax.random.split(jax.random.fold_in(key, 11))
    chan_draw = jax.random.uniform(chan_key, (ATTENTION_HEADS, KEY_CHANNELS), jnp.float32)
    head_draw = jax.random.uniform(head_key, (ATTENTION_HEADS,), jnp.float32)
    fast_heads = head_draw < 0.5
    low_end = jnp.where(fast_heads, 0.3, 4.5)[:, None]
    spread_width = jnp.where(fast_heads, 1.2, 2.0)[:, None]
    return (low_end + spread_width * chan_draw).reshape(ATTENTION_HEADS * KEY_CHANNELS).astype(jnp.float32)


def draw_decay_increment(key, part):
    where_key, depth_key = jax.random.split(jax.random.fold_in(key, 23))
    full_shape = (SEQS, LEN, ATTENTION_HEADS)
    struck = jax.random.uniform(where_key, full_shape, jnp.float32) < 3.0 / LEN
    depth = jax.random.uniform(depth_key, full_shape, jnp.float32, -0.69, -0.22)
    return jnp.where(struck, depth, 0.0).astype(jnp.float32)


def level_of(own_key, dims, shards, least, high):
    def one(dim, blocks):
        draws = jax.random.uniform(jax.random.fold_in(jax.random.fold_in(own_key, 6), dim), (blocks,), jnp.float32, least / len(shards), high / len(shards))
        return jnp.repeat(jnp.exp(draws), dims[dim] // blocks).reshape((-1,) + (1,) * (len(dims) - dim - 1))

    level = one(*shards[0])
    for cut in shards[1:]:
        level = level * one(*cut)
    return level


def bell_draw(own_key, extent, scale, bound, pieces=(), kind=jnp.bfloat16):
    loudness = level_of(own_key, extent, pieces, -0.22, 0.18) if pieces else 1.0
    entries = jax.random.normal(own_key, extent, jnp.float32) * scale * loudness
    return jnp.minimum(jnp.maximum(entries, -bound), bound).astype(kind)


def setup_inputs(seed: int = 0) -> dict:
    splits = jax.random.split(jax.random.key(seed), 14)
    return {
        "resid": bell_draw(splits[0], (SEQS, LEN, D), 1.0, 6.0, ((0, 16),)),
        "attention_norm_gain": jnp.clip(1.0 + 0.18 * jax.random.normal(splits[1], (D,), jnp.float32), 0.1, 1.9),
        "query_weight": bell_draw(splits[2], (D, ATTENTION_HEADS * KEY_CHANNELS), D ** -0.5, 0.125, ((0, 8), (1, 2))),
        "key_weight": bell_draw(splits[3], (D, ATTENTION_HEADS * KEY_CHANNELS), D ** -0.5, 0.125, ((0, 8), (1, 2))),
        "value_weight": bell_draw(splits[4], (D, ATTENTION_HEADS * HEAD_V), D ** -0.5, 0.125, ((0, 8), (1, 2))),
        "decay_down_weight": bell_draw(splits[5], (D, RANK), D ** -0.5, 0.125),
        "decay_up_weight": bell_draw(splits[6], (RANK, ATTENTION_HEADS * KEY_CHANNELS), RANK ** -0.5, 1.5),
        "decay_rate_bias": draw_decay_rate_bias(jax.random.fold_in(splits[13], 71), 0),
        "decay_increment": draw_decay_increment(jax.random.fold_in(splits[13], 71), 0),
        "head_norm_gain": jnp.clip(1.0 + 0.18 * jax.random.normal(splits[9], (HEAD_V,), jnp.float32), 0.1, 1.9),
        "feedforward_norm_gain": jnp.clip(1.0 + 0.18 * jax.random.normal(splits[10], (D,), jnp.float32), 0.1, 1.9),
        "up_weight": bell_draw(splits[11], (D, FF), D ** -0.5, 0.125, ((0, 8), (1, 2))),
        "down_weight": bell_draw(splits[12], (FF, D), FF ** -0.5, 0.09375, ((0, 2), (1, 8))),
    }


EPS = 1e-06
HIGH = lax.Precision.HIGHEST

def rms_rows(rows_in, gain_vec):
    values_f = rows_in.astype(jnp.float32)
    scaled = values_f * lax.rsqrt(lax.optimization_barrier(jnp.mean(values_f * values_f, axis=-1, keepdims=True)) + EPS)
    return (scaled * gain_vec).astype(jnp.bfloat16)

def project_heads(normed, weight, head_width):
    product = jnp.dot(normed, weight, preferred_element_type=jnp.float32)
    rounded = lax.optimization_barrier(product.astype(jnp.bfloat16)).astype(jnp.float32)
    return rounded.reshape(normed.shape[0], -1, head_width).transpose(1, 0, 2)

def gated_scan(queries, keys_in, values_in, logarithm_decay_rates):
    head_count, sequence_length, key_width = queries.shape
    value_width = values_in.shape[-1]
    blocks = sequence_length // BLOCK

    def split_blocks(source):
        return source.reshape(head_count, blocks, BLOCK, source.shape[-1]).transpose(1, 0, 2, 3)
    causal_mask = jnp.tril(jnp.ones((BLOCK, BLOCK), dtype=bool))

    def block_step(carry_state, input_tokens):
        q_blk, k_blk, v_blk, g_blk = input_tokens
        cumulative = jnp.cumsum(g_blk, axis=1)
        carried = jnp.einsum('hcd,hde->hce', q_blk * jnp.exp(cumulative), carry_state, precision=HIGH)
        log_gaps = cumulative[:, :, None, :] - cumulative[:, None, :, :]
        decays = jnp.exp(jnp.where(causal_mask[None, :, :, None], log_gaps, -jnp.inf))
        scores = lax.optimization_barrier(jnp.sum(q_blk[:, :, None, :] * k_blk[:, None, :, :] * decays, axis=-1))
        outputs = carried + jnp.einsum('hij,hje->hie', scores, v_blk, precision=HIGH)
        last_cum = cumulative[:, -1:, :]
        new_state = jnp.exp(last_cum[:, 0, :])[:, :, None] * carry_state + jnp.einsum('hcd,hce->hde', k_blk * jnp.exp(last_cum - cumulative), v_blk, precision=HIGH)
        return (new_state, outputs)
    start_state = jnp.zeros((head_count, key_width, value_width), jnp.float32)
    final_state, outputs = lax.scan(block_step, start_state, (split_blocks(queries), split_blocks(keys_in), split_blocks(values_in), split_blocks(logarithm_decay_rates)))
    return outputs.transpose(1, 0, 2, 3).reshape(head_count, sequence_length, value_width)

def reference(resid, attention_norm_gain, query_weight, key_weight, value_weight, decay_down_weight, decay_up_weight, decay_rate_bias, decay_increment, head_norm_gain, feedforward_norm_gain, up_weight, down_weight):

    def parts_sum(left_side, right_side, width):
        lefts = left_side.reshape(left_side.shape[0], N_TP, width).transpose(1, 0, 2)
        rights = right_side.reshape(N_TP, width, right_side.shape[1])

        def add_part(running, operands):
            partial_value = jnp.dot(operands[0], operands[1], preferred_element_type=jnp.float32)
            rounded = lax.optimization_barrier(partial_value.astype(jnp.bfloat16))
            return (running + rounded.astype(jnp.float32), None)
        zero_sum = jnp.zeros((left_side.shape[0], right_side.shape[1]), jnp.float32)
        return lax.scan(add_part, zero_sum, (lefts, rights))[0]

    def single_sequence(input_tokens):
        sequence_rows, decay_spike = input_tokens
        sequence_length = sequence_rows.shape[0]
        normed = rms_rows(sequence_rows, attention_norm_gain)
        queries = project_heads(normed, query_weight, KEY_CHANNELS) * KEY_CHANNELS ** (-0.5)
        keys_in = project_heads(normed, key_weight, KEY_CHANNELS)
        values_in = project_heads(normed, value_weight, HEAD_V)
        rate_low = jnp.dot(normed, decay_down_weight, preferred_element_type=jnp.float32).astype(jnp.bfloat16)
        decay_rate_logits = jnp.dot(rate_low, decay_up_weight, preferred_element_type=jnp.float32) + decay_rate_bias
        logarithm_decay_rates = (jax.nn.log_sigmoid(decay_rate_logits) / 16.0).reshape(sequence_length, ATTENTION_HEADS, KEY_CHANNELS) + decay_spike[:, :, None]
        head_out = gated_scan(queries, keys_in, values_in, logarithm_decay_rates.transpose(1, 0, 2))
        normalized = head_out * lax.rsqrt(lax.optimization_barrier(jnp.mean(head_out * head_out, axis=-1, keepdims=True)) + EPS) * head_norm_gain
        flat = normalized.transpose(1, 0, 2).reshape(sequence_length, ATTENTION_HEADS * HEAD_V)
        middle = (sequence_rows.astype(jnp.float32) + flat).astype(jnp.bfloat16)
        normed_mlp = rms_rows(middle, feedforward_norm_gain)
        up_acc = jnp.dot(normed_mlp, up_weight, preferred_element_type=jnp.float32)
        hidden = jnp.square(jax.nn.relu(up_acc)).astype(jnp.bfloat16)
        mlp_sum = parts_sum(hidden, down_weight, FF // N_TP)
        return (middle.astype(jnp.float32) + mlp_sum).astype(jnp.bfloat16)
    return lax.map(single_sequence, (resid, decay_increment))
```

```python
import functools

import jax
import jax.numpy as jnp
import numpy as np
from jax import lax
from jax.experimental import pallas as pl
from jax.experimental.pallas import tpu as pltpu
from jax.sharding import PartitionSpec as P

KEY_CHANNELS = 128
HEAD_V = 256
BLOCK = 64
FINE = 8
STRIDE = 4
ROWS = 128


EPS = 1e-06
MESH = pl.DeviceIdType.MESH
VMEM_LIMIT = 60 * 1024 * 1024


def rms_rows(rows_in, gain_vec):
    values_f = rows_in.astype(jnp.float32)
    scaled = values_f * lax.rsqrt(jnp.mean(values_f * values_f, axis=-1, keepdims=True) + EPS)
    return (scaled * gain_vec).astype(jnp.bfloat16)


def ring_to_fs(place, n):
    return jnp.where(place < n // 2, 2 * place, 2 * (n - 1 - place) + 1)


def fs_to_ring(fs, n):
    return jnp.where(lax.rem(fs, 2) == 0, fs // 2, n - 1 - fs // 2)


class Ring:
    def __init__(self, n, shards, held, full, sems):
        self.n, self.hops = n, n // 2
        self.shards, self.held, self.full = shards, held, full
        self.out_sem, self.in_sem, self.twin_out, self.twin_in, self.local = sems
        self.rep, self.fs, self.tp = (lax.axis_index(a) for a in ("rep", "fs", "tp"))
        self.me = fs_to_ring(self.fs, n)
        right = ring_to_fs(lax.rem(self.me + 1, n), n)
        left = ring_to_fs(lax.rem(self.me + n - 1, n), n)
        self.way_id = ((self.rep, right, self.tp), (self.rep, left, self.tp))
        self.twin_id = (1 - self.rep, self.fs, self.tp)

    def greet(self, others=()):
        barrier = pltpu.get_barrier_semaphore()
        who = (*self.way_id, self.twin_id, *others)
        for device in who:
            pl.semaphore_signal(barrier, inc=1, device_id=device, device_id_type=MESH)
        pl.semaphore_wait(barrier, len(who))

    def span(self, k, hop, way):
        half = self.held[k].shape[0] // 2
        source = ring_to_fs(lax.rem(self.me + (self.n - hop if way == 0 else hop), self.n), self.n)
        return source * (2 * half) + self.rep * half, half

    def cut(self, half, hop, way):
        if hop < self.hops - 1:
            return 0, half
        return (0, half // 2) if way == 0 else (half // 2, half - half // 2)

    def sending(self, k, hop, way):
        start, half = self.span(k, hop, way)
        shift, size = self.cut(half, hop, way)
        target = self.full[k].at[pl.ds(pl.multiple_of(start + shift, 16), size)]
        source = target
        if hop == 0:
            source = self.held[k].at[pl.ds(pl.multiple_of(self.rep * half + shift, 16), size)]
        return pltpu.make_async_remote_copy(
            src_ref=source,
            dst_ref=target,
            send_sem=self.out_sem.at[k, way, hop],
            recv_sem=self.in_sem.at[k, way, hop],
            device_id=self.way_id[way],
            device_id_type=MESH,
        )

    def landing(self, k, hop, way):
        start, half = self.span(k, hop + 1, way)
        shift, size = self.cut(half, hop, way)
        return self.full[k].at[pl.ds(pl.multiple_of(start + shift, 16), size)]

    def twin(self, k, hop, way):
        landed = self.landing(k, hop, way)
        return pltpu.make_async_remote_copy(
            src_ref=landed,
            dst_ref=landed,
            send_sem=self.twin_out.at[k, way, hop],
            recv_sem=self.twin_in.at[k, way, hop],
            device_id=self.twin_id,
            device_id_type=MESH,
        )

    def load(self, k):
        return pltpu.make_async_copy(self.shards[k], self.held[k], self.local.at[k, 0])

    def keep(self, k):
        rows = self.held[k].shape[0]
        at = pl.ds(pl.multiple_of(self.fs * rows, 16), rows)
        return pltpu.make_async_copy(self.held[k], self.full[k].at[at], self.local.at[k, 1])

    def start(self, others=()):
        count = len(self.held)
        for k in range(count):
            self.load(k).start()
        self.greet(others)
        for k in range(count):
            self.load(k).wait()
            for way in range(2):
                self.sending(k, 0, way).start()
        for k in range(count):
            self.keep(k).start()

    def events(self):
        return [(k, hop) for hop in range(self.hops) for k in range(len(self.held))]

    def event(self, k, hop):
        for way in range(2):
            landed = self.landing(k, hop, way)
            pltpu.make_async_remote_copy(
                src_ref=landed,
                dst_ref=landed,
                send_sem=self.out_sem.at[k, way, hop],
                recv_sem=self.in_sem.at[k, way, hop],
                device_id=self.way_id[way],
                device_id_type=MESH,
            ).wait_recv()
            if hop < self.hops - 1:
                self.sending(k, hop + 1, way).start()
            self.twin(k, hop, way).start()

    def finish(self):
        for k, hop in self.events():
            for way in range(2):
                self.sending(k, hop, way).wait_send()
                copy = self.twin(k, hop, way)
                copy.wait_send()
                start, half = self.span(k, hop + 1, way)
                other = start + (1 - 2 * self.rep) * half
                shift, size = self.cut(half, hop, way)
                there = self.full[k].at[pl.ds(pl.multiple_of(other + shift, 16), size)]
                pltpu.make_async_remote_copy(
                    src_ref=there,
                    dst_ref=there,
                    send_sem=self.twin_out.at[k, way, hop],
                    recv_sem=self.twin_in.at[k, way, hop],
                    device_id=self.twin_id,
                    device_id_type=MESH,
                ).wait_recv()
        for k in range(len(self.held)):
            self.keep(k).wait()


def ring_scratch(shards, n):
    count = len(shards)
    return [pltpu.VMEM(s.shape, s.dtype) for s in shards] + [
        pltpu.SemaphoreType.DMA((count, 2, n // 2)) for _ in range(4)
    ] + [pltpu.SemaphoreType.DMA((count, 2))]


def gathered_shapes(shards, n):
    return [jax.ShapeDtypeStruct((n * s.shape[0], s.shape[1]), s.dtype) for s in shards]


def gather_kernel(n, count, *refs):
    ring = Ring(n, refs[:count], refs[2 * count : 3 * count], refs[count : 2 * count], refs[3 * count :])
    ring.start()
    for k, hop in ring.events():
        ring.event(k, hop)
    ring.finish()


def ring_gather(shards, n, collective_id):
    count = len(shards)
    anywhere = pl.BlockSpec(memory_space=pl.ANY)
    return pl.pallas_call(
        functools.partial(gather_kernel, n, count),
        out_shape=gathered_shapes(shards, n),
        in_specs=[anywhere] * count,
        out_specs=[anywhere] * count,
        scratch_shapes=ring_scratch(shards, n),
        compiler_params=pltpu.CompilerParams(collective_id=collective_id, has_side_effects=True),
    )(*shards)


def decay_matrices():
    row = np.arange(BLOCK)[:, None]
    col = np.arange(BLOCK)[None, :]
    stack = [col <= row, col > row]
    half = BLOCK // 2
    while half >= FINE:
        ref = row // (2 * half) * (2 * half) + half - 1
        late = row % (2 * half) >= half
        stack.append(np.where(late, (col > ref) & (col <= row), (col > row) & (col <= ref)))
        half //= 2
    stack.append((col <= row) & (col // FINE == row // FINE))
    one = np.concatenate(stack, axis=0).astype(np.float32)
    return np.concatenate([one, one], axis=1)


def attention_block(
    heads,
    q_ref,
    k_ref,
    v_ref,
    low_ref,
    rate_ref,
    bias_ref,
    incr_ref,
    own_ref,
    gain_ref,
    sums_ref,
    spread_ref,
    out_ref,
    state,
):
    bf, f32 = jnp.bfloat16, jnp.float32
    logits = jnp.dot(low_ref[...], rate_ref[...], preferred_element_type=f32) + bias_ref[...]
    rates = (jnp.minimum(logits, 0.0) - jnp.log1p(jnp.exp(-jnp.abs(logits)))) * (1.0 / 16.0)
    increments = incr_ref[...]
    row = lax.broadcasted_iota(jnp.int32, (BLOCK, BLOCK), 0)
    col = lax.broadcasted_iota(jnp.int32, (BLOCK, BLOCK), 1)
    row_id = lax.broadcasted_iota(jnp.int32, (BLOCK, KEY_CHANNELS), 0)
    contract_last = (((1,), (1,)), ((), ()))
    for h in range(heads):
        keys_at = pl.ds(h * KEY_CHANNELS, KEY_CHANNELS)
        values_at = pl.ds(h * HEAD_V, HEAD_V)
        g = rates[:, h * KEY_CHANNELS : (h + 1) * KEY_CHANNELS] + increments[:, h : h + 1]
        high = g.astype(bf)
        low = (g - high.astype(f32)).astype(bf)
        sums = jnp.dot(
            sums_ref[...], jnp.concatenate([high, low], axis=0), preferred_element_type=f32
        )
        parts = [sums[i * BLOCK : (i + 1) * BLOCK] for i in range(sums.shape[0] // BLOCK)]
        q = q_ref[:, keys_at].astype(f32) * KEY_CHANNELS ** (-0.5)
        k = k_ref[:, keys_at].astype(f32)
        v = v_ref[:, values_at]
        from_start = jnp.exp(parts[0])
        fine = parts[-1]
        fine3 = fine.reshape(BLOCK // FINE, FINE, KEY_CHANNELS)
        k3 = k.reshape(BLOCK // FINE, FINE, KEY_CHANNELS)
        q3 = q.reshape(BLOCK // FINE, FINE, KEY_CHANNELS)
        terms = []
        for j in range(FINE):
            gap = jnp.minimum(fine3 - fine3[:, j : j + 1, :], 0.0)
            term = q3 * k3[:, j : j + 1, :] * jnp.exp(gap)
            terms.append(term.reshape(BLOCK, KEY_CHANNELS).astype(bf))
        scores = jnp.dot(
            jnp.concatenate(terms, axis=1), spread_ref[...], preferred_element_type=f32
        )
        scores = jnp.where((row // FINE == col // FINE) & (col <= row), scores, 0.0)
        half = BLOCK // 2
        for part in parts[2:-1]:
            near = jnp.exp(part)
            late = row_id % (2 * half) >= half
            q_side = jnp.where(late, q * near, 0.0).astype(bf)
            k_side = jnp.where(late, 0.0, k * near).astype(bf)
            level = lax.dot_general(q_side, k_side, contract_last, preferred_element_type=f32)
            scores += jnp.where(row // (2 * half) == col // (2 * half), level, 0.0)
            half //= 2
        carry = state[h]
        out = lax.dot_general(
            (q * from_start).astype(bf), carry.astype(bf), contract_last, preferred_element_type=f32
        ) + jnp.dot(scores.astype(bf), v, preferred_element_type=f32)
        to_end = (k * jnp.exp(parts[1])).astype(bf)
        state[h] = carry * from_start[BLOCK - 1 :, :] + lax.dot_general(
            v, to_end, (((0,), (0,)), ((), ())), preferred_element_type=f32
        )
        normalized = (
            out * lax.rsqrt(jnp.mean(out * out, axis=-1, keepdims=True) + EPS) * gain_ref[...]
        )
        out_ref[:, values_at] = (own_ref[:, values_at].astype(f32) + normalized).astype(bf)


def attend_kernel(n, heads, steps, n_tp, *refs):
    block_refs, shards, (middle, *full) = refs[:11], refs[11:13], refs[13:16]
    state, produced, out_sem, in_sem, own_sem = refs[16:21]
    held, sems = refs[21:23], refs[23:]
    width = produced.shape[1]
    step = pl.program_id(0)
    ring = Ring(n, shards, held, full, sems)
    ids = [(ring.rep, ring.fs, lax.rem(ring.tp + d, n_tp)) for d in range(1, n_tp)]

    def piece(part, owner):
        rows = pl.ds(pl.multiple_of(part * BLOCK, BLOCK), BLOCK)
        columns = pl.ds(pl.multiple_of(owner * width, KEY_CHANNELS), width)
        return produced.at[rows], middle.at[rows, columns]

    def passing(part, d):
        source, target = piece(part, ring.tp)
        return pltpu.make_async_remote_copy(
            src_ref=source,
            dst_ref=target,
            send_sem=out_sem.at[part, d - 1],
            recv_sem=in_sem.at[part, d - 1],
            device_id=ids[d - 1],
            device_id_type=MESH,
        )

    def keeping(part):
        source, target = piece(part, ring.tp)
        return pltpu.make_async_copy(source, target, own_sem.at[part])

    def hand_out(part):
        for d in range(1, n_tp):
            passing(part, d).start()
        keeping(part).start()

    @pl.when(step == 0)
    def _():
        ring.start(ids)
        state[...] = jnp.zeros_like(state)

    @pl.when(step > 0)
    def _():
        hand_out(step - 1)

    events = ring.events()
    late = [e for i, e in enumerate(events) if (i + 1) * STRIDE >= steps]
    for i, (k, hop) in enumerate(events):
        if (k, hop) not in late:

            @pl.when(step == (i + 1) * STRIDE)
            def _(k=k, hop=hop):
                ring.event(k, hop)

    rows = pl.ds(pl.multiple_of(step * BLOCK, BLOCK), BLOCK)
    attention_block(heads, *block_refs, produced.at[rows], state)

    @pl.when(step == steps - 1)
    def _():
        hand_out(step)
        for k, hop in late:
            ring.event(k, hop)
        ring.finish()

        @pl.loop(0, steps)
        def _(part):
            for d in range(1, n_tp):
                passing(part, d).wait_send()
                _, there = piece(part, lax.rem(ring.tp + n_tp - d, n_tp))
                pltpu.make_async_remote_copy(
                    src_ref=there,
                    dst_ref=there,
                    send_sem=out_sem.at[part, d - 1],
                    recv_sem=in_sem.at[part, d - 1],
                    device_id=ids[d - 1],
                    device_id_type=MESH,
                ).wait_recv()
            keeping(part).wait()


def attend(q, k, v, rate_low, rate_cols, bias_cols, increments, own_cols, head_gain, shards, n, n_tp):
    length, width_qk = q.shape
    heads = width_qk // KEY_CHANNELS
    width_v = v.shape[1]
    steps = length // BLOCK
    sums = jnp.asarray(decay_matrices(), jnp.bfloat16)
    lane = np.arange(FINE * KEY_CHANNELS)[:, None] // KEY_CHANNELS
    spread = jnp.asarray(lane == np.arange(BLOCK)[None, :] % FINE, jnp.bfloat16)

    def rows(width):
        return pl.BlockSpec((BLOCK, width), lambda i: (i, 0))

    def whole(array):
        return pl.BlockSpec(array.shape, lambda i: (0, 0))

    bias_row, gain_row = bias_cols[None], head_gain[None]
    anywhere = pl.BlockSpec(memory_space=pl.ANY)
    peers = max(n_tp - 1, 1)
    return pl.pallas_call(
        functools.partial(attend_kernel, n, heads, steps, n_tp),
        grid=(steps,),
        out_shape=[jax.ShapeDtypeStruct((length, width_v * n_tp), jnp.bfloat16)]
        + gathered_shapes(shards, n),
        in_specs=[
            rows(width_qk),
            rows(width_qk),
            rows(width_v),
            rows(rate_low.shape[1]),
            whole(rate_cols),
            whole(bias_row),
            rows(heads),
            rows(width_v),
            whole(gain_row),
            whole(sums),
            whole(spread),
            anywhere,
            anywhere,
        ],
        out_specs=[anywhere] * 3,
        scratch_shapes=[
            pltpu.VMEM((heads, HEAD_V, KEY_CHANNELS), jnp.float32),
            pltpu.VMEM((length, width_v), jnp.bfloat16),
            pltpu.SemaphoreType.DMA((steps, peers)),
            pltpu.SemaphoreType.DMA((steps, peers)),
            pltpu.SemaphoreType.DMA((steps,)),
        ]
        + ring_scratch(shards, n),
        compiler_params=pltpu.CompilerParams(
            collective_id=2, has_side_effects=True, vmem_limit_bytes=VMEM_LIMIT
        ),
    )(q, k, v, rate_low, rate_cols, bias_row, increments, own_cols, gain_row, sums, spread, *shards)


def feed_kernel(n, n_tp, chunks, middle_ref, gain_ref, up_ref, down_ref, out_ref, *scratch):
    up, down, total, sent, came, load_sem, out_sem, in_sem = scratch
    rep, fs, tp = (lax.axis_index(a) for a in ("rep", "fs", "tp"))
    ids = [(rep, fs, lax.rem(tp + d, n_tp)) for d in range(1, n_tp)]
    step = pl.program_id(0)
    hidden_width = up.shape[1]
    block = down.shape[1]
    width = total.shape[1]
    per_owner = n // n_tp
    loads = (
        pltpu.make_async_copy(up_ref, up, load_sem.at[0]),
        pltpu.make_async_copy(down_ref, down, load_sem.at[1]),
    )

    def passing(part, d):
        rows = pl.ds(pl.multiple_of(part * ROWS, ROWS), ROWS)
        return pltpu.make_async_remote_copy(
            src_ref=sent.at[lax.rem(tp + d, n_tp), rows],
            dst_ref=came.at[tp, rows],
            send_sem=out_sem.at[part, d - 1],
            recv_sem=in_sem.at[part, d - 1],
            device_id=ids[d - 1],
            device_id_type=MESH,
        )

    @pl.when(step == 0)
    def _():
        for load in loads:
            load.start()
        barrier = pltpu.get_barrier_semaphore()
        for device in ids:
            pl.semaphore_signal(barrier, inc=1, device_id=device, device_id_type=MESH)
        pl.semaphore_wait(barrier, n_tp - 1)
        loads[0].wait()

    @pl.when(step > 0)
    def _():
        for d in range(1, n_tp):
            passing(step - 1, d).start()

    rows = pl.ds(pl.multiple_of(step * ROWS, ROWS), ROWS)
    normed = rms_rows(middle_ref[...], gain_ref[...])
    acc = jnp.dot(normed, up[...], preferred_element_type=jnp.float32)
    hidden = jnp.square(jnp.maximum(acc, 0.0)).astype(jnp.bfloat16)

    @pl.when(step == 0)
    def _():
        loads[1].wait()

    for i in range(n):
        term = jnp.dot(
            hidden,
            down[i * hidden_width : (i + 1) * hidden_width, :],
            preferred_element_type=jnp.float32,
        )
        at = (i % per_owner) * block
        sent[i // per_owner, rows, at : at + block] = term.astype(jnp.bfloat16)
    own_at = pl.ds(pl.multiple_of(tp * width, KEY_CHANNELS), width)
    total[rows, :] = middle_ref[:, own_at].astype(jnp.float32) + sent[tp, rows, :].astype(jnp.float32)

    @pl.when(step == chunks - 1)
    def _():
        for d in range(1, n_tp):
            passing(step, d).start()

        @pl.loop(0, chunks)
        def _(part):
            at = pl.ds(pl.multiple_of(part * ROWS, ROWS), ROWS)
            summed = total[at, :]
            for d in range(1, n_tp):
                passing(part, d).wait_send()
                source = lax.rem(tp + n_tp - d, n_tp)
                there = came.at[source, at]
                pltpu.make_async_remote_copy(
                    src_ref=there,
                    dst_ref=there,
                    send_sem=out_sem.at[part, d - 1],
                    recv_sem=in_sem.at[part, d - 1],
                    device_id=ids[d - 1],
                    device_id_type=MESH,
                ).wait_recv()
                summed += came[source, at, :].astype(jnp.float32)
            out_ref[at, :] = summed.astype(jnp.bfloat16)


def feed_forward(middle, gain, up, down, n, n_tp):
    length, features = middle.shape
    width = features // n_tp
    chunks = length // ROWS
    peers = max(n_tp - 1, 1)
    anywhere = pl.BlockSpec(memory_space=pl.ANY)
    return pl.pallas_call(
        functools.partial(feed_kernel, n, n_tp, chunks),
        grid=(chunks,),
        out_shape=jax.ShapeDtypeStruct((length, width), jnp.bfloat16),
        in_specs=[
            pl.BlockSpec((ROWS, features), lambda i: (i, 0)),
            pl.BlockSpec((1, features), lambda i: (0, 0)),
            anywhere,
            anywhere,
        ],
        out_specs=pl.BlockSpec((length, width), lambda i: (0, 0)),
        scratch_shapes=[
            pltpu.VMEM(up.shape, up.dtype),
            pltpu.VMEM(down.shape, down.dtype),
            pltpu.VMEM((length, width), jnp.float32),
            pltpu.VMEM((n_tp, length, width), jnp.bfloat16),
            pltpu.VMEM((n_tp, length, width), jnp.bfloat16),
            pltpu.SemaphoreType.DMA((2,)),
            pltpu.SemaphoreType.DMA((chunks, peers)),
            pltpu.SemaphoreType.DMA((chunks, peers)),
        ],
        compiler_params=pltpu.CompilerParams(
            collective_id=3, has_side_effects=True, vmem_limit_bytes=VMEM_LIMIT
        ),
    )(middle, gain[None], up, down)


def per_device(
    n,
    n_tp,
    resid,
    attention_norm_gain,
    query_weight,
    key_weight,
    value_weight,
    decay_down_weight,
    decay_up_weight,
    decay_rate_bias,
    decay_increment,
    head_norm_gain,
    feedforward_norm_gain,
    up_weight,
    down_weight,
):
    sequence_rows = resid[0]
    col_width = value_weight.shape[1]
    width_qk = query_weight.shape[1]
    own_cols = lax.dynamic_slice_in_dim(sequence_rows, lax.axis_index("tp") * col_width, col_width, 1)
    query_full, key_full, value_full = ring_gather((query_weight, key_weight, value_weight), n, 1)
    normed = rms_rows(sequence_rows, attention_norm_gain)
    q, k, v = (
        jnp.dot(normed, weight, preferred_element_type=jnp.float32).astype(jnp.bfloat16)
        for weight in (query_full, key_full, value_full)
    )
    first_col = lax.axis_index("tp") * width_qk
    rate_cols = lax.dynamic_slice_in_dim(decay_up_weight, first_col, width_qk, 1)
    bias_cols = lax.dynamic_slice_in_dim(decay_rate_bias, first_col, width_qk, 0)
    rate_low = jnp.dot(normed, decay_down_weight, preferred_element_type=jnp.float32).astype(
        jnp.bfloat16
    )
    middle, up_full, down_full = attend(
        q,
        k,
        v,
        rate_low,
        rate_cols,
        bias_cols,
        decay_increment[0],
        own_cols,
        head_norm_gain,
        (up_weight, down_weight),
        n,
        n_tp,
    )
    return feed_forward(middle, feedforward_norm_gain, up_full, down_full, n, n_tp)[None]


def solution(mesh):
    return jax.shard_map(
        functools.partial(per_device, mesh.shape["fs"], mesh.shape["tp"]),
        mesh=mesh,
        in_specs=(
            P(("rep", "fs"), None, None),
            P(),
            P("fs", "tp"),
            P("fs", "tp"),
            P("fs", "tp"),
            P(),
            P(),
            P(),
            P(("rep", "fs"), None, "tp"),
            P(),
            P(),
            P("fs", "tp"),
            P("tp", "fs"),
        ),
        out_specs=P(("rep", "fs"), None, "tp"),
        check_vma=False,
    )
```

```python
import functools

import jax
import jax.numpy as jnp
import numpy as np
from jax import lax
from jax.experimental import pallas as pl
from jax.experimental.pallas import tpu as pltpu
from jax.sharding import PartitionSpec as P

KEY_CHANNELS = 128
HEAD_V = 256
BLOCK = 64
FINE = 8
STRIDE = 4
ROWS = 128


EPS = 1e-06
MESH = pl.DeviceIdType.MESH
VMEM_LIMIT = 60 * 1024 * 1024


def rms_rows(rows_in, gain_vec):
    values_f = rows_in.astype(jnp.float32)
    scaled = values_f * lax.rsqrt(jnp.mean(values_f * values_f, axis=-1, keepdims=True) + EPS)
    return (scaled * gain_vec).astype(jnp.bfloat16)


def ring_to_fs(place, n):
    return jnp.where(place < n // 2, 2 * place, 2 * (n - 1 - place) + 1)


def fs_to_ring(fs, n):
    return jnp.where(lax.rem(fs, 2) == 0, fs // 2, n - 1 - fs // 2)


class Ring:
    def __init__(self, n, shards, held, full, sems):
        self.n, self.hops = n, n // 2
        self.shards, self.held, self.full = shards, held, full
        self.out_sem, self.in_sem, self.twin_out, self.twin_in, self.local = sems
        self.rep, self.fs, self.tp = (lax.axis_index(a) for a in ("rep", "fs", "tp"))
        self.me = fs_to_ring(self.fs, n)
        right = ring_to_fs(lax.rem(self.me + 1, n), n)
        left = ring_to_fs(lax.rem(self.me + n - 1, n), n)
        self.way_id = ((self.rep, right, self.tp), (self.rep, left, self.tp))
        self.twin_id = (1 - self.rep, self.fs, self.tp)

    def greet(self, others=()):
        barrier = pltpu.get_barrier_semaphore()
        who = (*self.way_id, self.twin_id, *others)
        for device in who:
            pl.semaphore_signal(barrier, inc=1, device_id=device, device_id_type=MESH)
        pl.semaphore_wait(barrier, len(who))

    def span(self, k, hop, way):
        half = self.held[k].shape[0] // 2
        source = ring_to_fs(lax.rem(self.me + (self.n - hop if way == 0 else hop), self.n), self.n)
        return source * (2 * half) + self.rep * half, half

    def cut(self, half, hop, way):
        if hop < self.hops - 1:
            return 0, half
        return (0, half // 2) if way == 0 else (half // 2, half - half // 2)

    def sending(self, k, hop, way):
        start, half = self.span(k, hop, way)
        shift, size = self.cut(half, hop, way)
        target = self.full[k].at[pl.ds(pl.multiple_of(start + shift, 16), size)]
        source = target
        if hop == 0:
            source = self.held[k].at[pl.ds(pl.multiple_of(self.rep * half + shift, 16), size)]
        return pltpu.make_async_remote_copy(
            src_ref=source,
            dst_ref=target,
            send_sem=self.out_sem.at[k, way, hop],
            recv_sem=self.in_sem.at[k, way, hop],
            device_id=self.way_id[way],
            device_id_type=MESH,
        )

    def landing(self, k, hop, way):
        start, half = self.span(k, hop + 1, way)
        shift, size = self.cut(half, hop, way)
        return self.full[k].at[pl.ds(pl.multiple_of(start + shift, 16), size)]

    def twin(self, k, hop, way):
        landed = self.landing(k, hop, way)
        return pltpu.make_async_remote_copy(
            src_ref=landed,
            dst_ref=landed,
            send_sem=self.twin_out.at[k, way, hop],
            recv_sem=self.twin_in.at[k, way, hop],
            device_id=self.twin_id,
            device_id_type=MESH,
        )

    def load(self, k):
        return pltpu.make_async_copy(self.shards[k], self.held[k], self.local.at[k, 0])

    def keep(self, k):
        rows = self.held[k].shape[0]
        at = pl.ds(pl.multiple_of(self.fs * rows, 16), rows)
        return pltpu.make_async_copy(self.held[k], self.full[k].at[at], self.local.at[k, 1])

    def start(self, others=()):
        count = len(self.held)
        for k in range(count):
            self.load(k).start()
        self.greet(others)
        for k in range(count):
            self.load(k).wait()
            for way in range(2):
                self.sending(k, 0, way).start()
        for k in range(count):
            self.keep(k).start()

    def events(self):
        return [(k, hop) for hop in range(self.hops) for k in range(len(self.held))]

    def event(self, k, hop):
        for way in range(2):
            landed = self.landing(k, hop, way)
            pltpu.make_async_remote_copy(
                src_ref=landed,
                dst_ref=landed,
                send_sem=self.out_sem.at[k, way, hop],
                recv_sem=self.in_sem.at[k, way, hop],
                device_id=self.way_id[way],
                device_id_type=MESH,
            ).wait_recv()
            if hop < self.hops - 1:
                self.sending(k, hop + 1, way).start()
            self.twin(k, hop, way).start()

    def twin_arrived(self, k, hop, way):
        start, half = self.span(k, hop + 1, way)
        other = start + (1 - 2 * self.rep) * half
        shift, size = self.cut(half, hop, way)
        there = self.full[k].at[pl.ds(pl.multiple_of(other + shift, 16), size)]
        pltpu.make_async_remote_copy(
            src_ref=there,
            dst_ref=there,
            send_sem=self.twin_out.at[k, way, hop],
            recv_sem=self.twin_in.at[k, way, hop],
            device_id=self.twin_id,
            device_id_type=MESH,
        ).wait_recv()

    def sent(self):
        for k, hop in self.events():
            for way in range(2):
                self.sending(k, hop, way).wait_send()
                self.twin(k, hop, way).wait_send()
        for k in range(len(self.held)):
            self.keep(k).wait()

    def finish(self):
        for k, hop in self.events():
            for way in range(2):
                self.twin_arrived(k, hop, way)
        self.sent()


def ring_scratch(shards, n):
    count = len(shards)
    return [pltpu.VMEM(s.shape, s.dtype) for s in shards] + [
        pltpu.SemaphoreType.DMA((count, 2, n // 2)) for _ in range(4)
    ] + [pltpu.SemaphoreType.DMA((count, 2))]


def gathered_shapes(shards, n):
    return [jax.ShapeDtypeStruct((n * s.shape[0], s.shape[1]), s.dtype) for s in shards]


def gather_kernel(n, count, *refs):
    ring = Ring(n, refs[:count], refs[2 * count : 3 * count], refs[count : 2 * count], refs[3 * count :])
    ring.start()
    for k, hop in ring.events():
        ring.event(k, hop)
    ring.finish()


def ring_gather(shards, n, collective_id):
    count = len(shards)
    anywhere = pl.BlockSpec(memory_space=pl.ANY)
    return pl.pallas_call(
        functools.partial(gather_kernel, n, count),
        out_shape=gathered_shapes(shards, n),
        in_specs=[anywhere] * count,
        out_specs=[anywhere] * count,
        scratch_shapes=ring_scratch(shards, n),
        compiler_params=pltpu.CompilerParams(collective_id=collective_id, has_side_effects=True),
    )(*shards)


def decay_matrices():
    row = np.arange(BLOCK)[:, None]
    col = np.arange(BLOCK)[None, :]
    stack = [col <= row, col > row]
    half = BLOCK // 2
    while half >= FINE:
        ref = row // (2 * half) * (2 * half) + half - 1
        late = row % (2 * half) >= half
        stack.append(np.where(late, (col > ref) & (col <= row), (col > row) & (col <= ref)))
        half //= 2
    stack.append((col <= row) & (col // FINE == row // FINE))
    one = np.concatenate(stack, axis=0).astype(np.float32)
    return np.concatenate([one, one], axis=1)


def attention_block(
    heads,
    q_ref,
    k_ref,
    v_ref,
    low_ref,
    rate_ref,
    bias_ref,
    incr_ref,
    own_ref,
    gain_ref,
    sums_ref,
    spread_ref,
    out_ref,
    state,
):
    bf, f32 = jnp.bfloat16, jnp.float32
    logits = jnp.dot(low_ref[...], rate_ref[...], preferred_element_type=f32) + bias_ref[...]
    rates = (jnp.minimum(logits, 0.0) - jnp.log1p(jnp.exp(-jnp.abs(logits)))) * (1.0 / 16.0)
    increments = incr_ref[...]
    row = lax.broadcasted_iota(jnp.int32, (BLOCK, BLOCK), 0)
    col = lax.broadcasted_iota(jnp.int32, (BLOCK, BLOCK), 1)
    row_id = lax.broadcasted_iota(jnp.int32, (BLOCK, KEY_CHANNELS), 0)
    contract_last = (((1,), (1,)), ((), ()))
    for h in range(heads):
        keys_at = pl.ds(h * KEY_CHANNELS, KEY_CHANNELS)
        values_at = pl.ds(h * HEAD_V, HEAD_V)
        g = rates[:, h * KEY_CHANNELS : (h + 1) * KEY_CHANNELS] + increments[:, h : h + 1]
        high = g.astype(bf)
        low = (g - high.astype(f32)).astype(bf)
        sums = jnp.dot(
            sums_ref[...], jnp.concatenate([high, low], axis=0), preferred_element_type=f32
        )
        parts = [sums[i * BLOCK : (i + 1) * BLOCK] for i in range(sums.shape[0] // BLOCK)]
        q = q_ref[:, keys_at].astype(f32) * KEY_CHANNELS ** (-0.5)
        k = k_ref[:, keys_at].astype(f32)
        v = v_ref[:, values_at]
        from_start = jnp.exp(parts[0])
        fine = parts[-1]
        fine3 = fine.reshape(BLOCK // FINE, FINE, KEY_CHANNELS)
        k3 = k.reshape(BLOCK // FINE, FINE, KEY_CHANNELS)
        q3 = q.reshape(BLOCK // FINE, FINE, KEY_CHANNELS)
        terms = []
        for j in range(FINE):
            gap = jnp.minimum(fine3 - fine3[:, j : j + 1, :], 0.0)
            term = q3 * k3[:, j : j + 1, :] * jnp.exp(gap)
            terms.append(term.reshape(BLOCK, KEY_CHANNELS).astype(bf))
        scores = jnp.dot(
            jnp.concatenate(terms, axis=1), spread_ref[...], preferred_element_type=f32
        )
        scores = jnp.where((row // FINE == col // FINE) & (col <= row), scores, 0.0)
        half = BLOCK // 2
        for part in parts[2:-1]:
            near = jnp.exp(part)
            late = row_id % (2 * half) >= half
            q_side = jnp.where(late, q * near, 0.0).astype(bf)
            k_side = jnp.where(late, 0.0, k * near).astype(bf)
            level = lax.dot_general(q_side, k_side, contract_last, preferred_element_type=f32)
            scores += jnp.where(row // (2 * half) == col // (2 * half), level, 0.0)
            half //= 2
        carry = state[h]
        out = lax.dot_general(
            (q * from_start).astype(bf), carry.astype(bf), contract_last, preferred_element_type=f32
        ) + jnp.dot(scores.astype(bf), v, preferred_element_type=f32)
        to_end = (k * jnp.exp(parts[1])).astype(bf)
        state[h] = carry * from_start[BLOCK - 1 :, :] + lax.dot_general(
            v, to_end, (((0,), (0,)), ((), ())), preferred_element_type=f32
        )
        normalized = (
            out * lax.rsqrt(jnp.mean(out * out, axis=-1, keepdims=True) + EPS) * gain_ref[...]
        )
        own_at = pl.ds(pl.multiple_of(lax.axis_index("tp") * heads * HEAD_V + h * HEAD_V, 128), HEAD_V)
        out_ref[:, values_at] = (own_ref[:, own_at].astype(f32) + normalized).astype(bf)


def attend_kernel(n, heads, steps, n_tp, *refs):
    block_refs, shards, (middle, *full) = refs[:11], refs[11:12], refs[12:14]
    state, produced, out_sem, in_sem, own_sem = refs[14:19]
    held, sems = refs[19:20], refs[20:]
    width = produced.shape[1]
    step = pl.program_id(0)
    ring = Ring(n, shards, held, full, sems)
    ids = [(ring.rep, ring.fs, lax.rem(ring.tp + d, n_tp)) for d in range(1, n_tp)]

    def piece(part, owner):
        rows = pl.ds(pl.multiple_of(part * BLOCK, BLOCK), BLOCK)
        columns = pl.ds(pl.multiple_of(owner * width, KEY_CHANNELS), width)
        return produced.at[rows], middle.at[rows, columns]

    def passing(part, d):
        source, target = piece(part, ring.tp)
        return pltpu.make_async_remote_copy(
            src_ref=source,
            dst_ref=target,
            send_sem=out_sem.at[part, d - 1],
            recv_sem=in_sem.at[part, d - 1],
            device_id=ids[d - 1],
            device_id_type=MESH,
        )

    def keeping(part):
        source, target = piece(part, ring.tp)
        return pltpu.make_async_copy(source, target, own_sem.at[part])

    def hand_out(part):
        for d in range(1, n_tp):
            passing(part, d).start()
        keeping(part).start()

    @pl.when(step == 0)
    def _():
        ring.start(ids)
        state[...] = jnp.zeros_like(state)

    @pl.when(step > 0)
    def _():
        hand_out(step - 1)

    events = ring.events()
    late = [e for i, e in enumerate(events) if (i + 1) * STRIDE >= steps]
    for i, (k, hop) in enumerate(events):
        if (k, hop) not in late:

            @pl.when(step == (i + 1) * STRIDE)
            def _(k=k, hop=hop):
                ring.event(k, hop)

    rows = pl.ds(pl.multiple_of(step * BLOCK, BLOCK), BLOCK)
    attention_block(heads, *block_refs, produced.at[rows], state)

    @pl.when(step == steps - 1)
    def _():
        hand_out(step)
        for k, hop in late:
            ring.event(k, hop)
        ring.finish()

        @pl.loop(0, steps)
        def _(part):
            for d in range(1, n_tp):
                passing(part, d).wait_send()
                _, there = piece(part, lax.rem(ring.tp + n_tp - d, n_tp))
                pltpu.make_async_remote_copy(
                    src_ref=there,
                    dst_ref=there,
                    send_sem=out_sem.at[part, d - 1],
                    recv_sem=in_sem.at[part, d - 1],
                    device_id=ids[d - 1],
                    device_id_type=MESH,
                ).wait_recv()
            keeping(part).wait()


def attend(q, k, v, rate_low, rate_cols, bias_cols, increments, own_cols, head_gain, shards, n, n_tp):
    length, width_qk = q.shape
    heads = width_qk // KEY_CHANNELS
    width_v = v.shape[1]
    steps = length // BLOCK
    sums = jnp.asarray(decay_matrices(), jnp.bfloat16)
    lane = np.arange(FINE * KEY_CHANNELS)[:, None] // KEY_CHANNELS
    spread = jnp.asarray(lane == np.arange(BLOCK)[None, :] % FINE, jnp.bfloat16)

    def rows(width):
        return pl.BlockSpec((BLOCK, width), lambda i: (i, 0))

    def whole(array):
        return pl.BlockSpec(array.shape, lambda i: (0, 0))

    bias_row, gain_row = bias_cols[None], head_gain[None]
    anywhere = pl.BlockSpec(memory_space=pl.ANY)
    peers = max(n_tp - 1, 1)
    return pl.pallas_call(
        functools.partial(attend_kernel, n, heads, steps, n_tp),
        grid=(steps,),
        out_shape=[jax.ShapeDtypeStruct((length, width_v * n_tp), jnp.bfloat16)]
        + gathered_shapes(shards, n),
        in_specs=[
            rows(width_qk),
            rows(width_qk),
            rows(width_v),
            rows(rate_low.shape[1]),
            whole(rate_cols),
            whole(bias_row),
            rows(heads),
            rows(width_v * n_tp),
            whole(gain_row),
            whole(sums),
            whole(spread),
            anywhere,
        ],
        out_specs=[anywhere] * 2,
        scratch_shapes=[
            pltpu.VMEM((heads, HEAD_V, KEY_CHANNELS), jnp.float32),
            pltpu.VMEM((length, width_v), jnp.bfloat16),
            pltpu.SemaphoreType.DMA((steps, peers)),
            pltpu.SemaphoreType.DMA((steps, peers)),
            pltpu.SemaphoreType.DMA((steps,)),
        ]
        + ring_scratch(shards, n),
        compiler_params=pltpu.CompilerParams(
            collective_id=2, has_side_effects=True, vmem_limit_bytes=VMEM_LIMIT
        ),
    )(q, k, v, rate_low, rate_cols, bias_row, increments, own_cols, gain_row, sums, spread, *shards)


def feed_kernel(n, n_tp, middle, gain_ref, up_ref, down_ref, out_ref, down_full, *scratch):
    up, hidden, block_buf, terms, came, load_sem, block_sem, out_sem, in_sem = scratch[:9]
    ring = Ring(n, (down_ref,), scratch[9:10], (down_full,), scratch[10:])
    rep, fs, tp = ring.rep, ring.fs, ring.tp
    peers = [(rep, fs, lax.rem(tp + d, n_tp)) for d in range(1, n_tp)]
    length = hidden.shape[0]
    depth, block = block_buf.shape[1:]
    per_owner = n // n_tp
    width = per_owner * block
    load = pltpu.make_async_copy(up_ref, up, load_sem)
    load.start()
    ring.start(peers)
    load.wait()

    def chunk(part):
        return pl.ds(pl.multiple_of(part * ROWS, ROWS), ROWS)

    @pl.loop(0, length // ROWS)
    def _(part):
        normed = rms_rows(middle[chunk(part), :], gain_ref[...])
        acc = jnp.dot(normed, up[...], preferred_element_type=jnp.float32)
        hidden[chunk(part), :] = jnp.square(jnp.maximum(acc, 0.0)).astype(jnp.bfloat16)

    def fetch(owner, slot):
        at = pl.ds(pl.multiple_of(owner * depth, 16), depth)
        return pltpu.make_async_copy(down_full.at[at], block_buf.at[slot], block_sem.at[slot])

    def multiply(owner, weights):
        @pl.loop(0, length // (2 * ROWS))
        def _(part):
            at = pl.ds(pl.multiple_of(part * 2 * ROWS, ROWS), 2 * ROWS)
            term = jnp.dot(hidden[at, :], weights[...], preferred_element_type=jnp.float32)
            terms[owner, at, :] = term.astype(jnp.bfloat16)

    def passing(owner):
        target = owner // per_owner
        return pltpu.make_async_remote_copy(
            src_ref=terms.at[owner],
            dst_ref=came.at[tp, owner - target * per_owner],
            send_sem=out_sem.at[owner],
            recv_sem=in_sem.at[tp, owner - target * per_owner],
            device_id=(rep, fs, target),
            device_id_type=MESH,
        )

    def hand_out(owner):
        @pl.when(owner // per_owner != tp)
        def _():
            passing(owner).start()

    multiply(fs, ring.held[0])
    for hop in range(ring.hops):
        ring.event(0, hop)
        if hop == 0:
            hand_out(fs)
        for way in range(2):
            ring.twin_arrived(0, hop, way)
        ways = 2 if hop < ring.hops - 1 else 1
        owners = [
            ring_to_fs(lax.rem(ring.me + (n - hop - 1 if way == 0 else hop + 1), n), n)
            for way in range(ways)
        ]
        for way, owner in enumerate(owners):
            fetch(owner, way).start()
        for way, owner in enumerate(owners):
            fetch(owner, way).wait()
            multiply(owner, block_buf.at[way])
        for owner in owners:
            hand_out(owner)
    ring.sent()

    @pl.loop(0, n)
    def _(owner):
        @pl.when(owner // per_owner != tp)
        def _():
            passing(owner).wait_send()

    for j in range(per_owner):
        for d in range(1, n_tp):
            source = lax.rem(tp + d, n_tp)
            there = came.at[source, j]
            pltpu.make_async_remote_copy(
                src_ref=there,
                dst_ref=there,
                send_sem=out_sem.at[j],
                recv_sem=in_sem.at[source, j],
                device_id=peers[0],
                device_id_type=MESH,
            ).wait_recv()

    own_at = pl.ds(pl.multiple_of(tp * width, KEY_CHANNELS), width)

    @pl.loop(0, length // ROWS)
    def _(part):
        own = middle[chunk(part), own_at].astype(jnp.float32)
        for j in range(per_owner):
            columns = slice(j * block, (j + 1) * block)
            summed = own[:, columns] + terms[tp * per_owner + j, chunk(part), :].astype(jnp.float32)
            for d in range(1, n_tp):
                source = lax.rem(tp + d, n_tp)
                summed += came[source, j, chunk(part), :].astype(jnp.float32)
            out_ref[chunk(part), columns] = summed.astype(jnp.bfloat16)


def feed_forward(middle, gain, up, down, n, n_tp):
    length, features = middle.shape
    width = features // n_tp
    depth, block = down.shape
    anywhere = pl.BlockSpec(memory_space=pl.ANY)
    vmem = pl.BlockSpec(memory_space=pltpu.VMEM)
    bf = jnp.bfloat16
    return pl.pallas_call(
        functools.partial(feed_kernel, n, n_tp),
        out_shape=[jax.ShapeDtypeStruct((length, width), bf)] + gathered_shapes((down,), n),
        in_specs=[vmem, vmem, anywhere, anywhere],
        out_specs=[vmem, anywhere],
        scratch_shapes=[
            pltpu.VMEM(up.shape, bf),
            pltpu.VMEM((length, up.shape[1]), bf),
            pltpu.VMEM((2, depth, block), bf),
            pltpu.VMEM((n, length, block), bf),
            pltpu.VMEM((n_tp, n // n_tp, length, block), bf),
            pltpu.SemaphoreType.DMA,
            pltpu.SemaphoreType.DMA((2,)),
            pltpu.SemaphoreType.DMA((n,)),
            pltpu.SemaphoreType.DMA((n_tp, n // n_tp)),
        ]
        + ring_scratch((down,), n),
        compiler_params=pltpu.CompilerParams(
            collective_id=3, has_side_effects=True, vmem_limit_bytes=VMEM_LIMIT
        ),
    )(middle, gain[None], up, down)[0]


def per_device(
    n,
    n_tp,
    resid,
    attention_norm_gain,
    query_weight,
    key_weight,
    value_weight,
    decay_down_weight,
    decay_up_weight,
    decay_rate_bias,
    decay_increment,
    head_norm_gain,
    feedforward_norm_gain,
    up_weight,
    down_weight,
):
    sequence_rows = resid[0]
    width_qk = query_weight.shape[1]
    query_full, key_full, value_full = ring_gather((query_weight, key_weight, value_weight), n, 1)
    normed = rms_rows(sequence_rows, attention_norm_gain)
    q, k, v = (
        jnp.dot(normed, weight, preferred_element_type=jnp.float32).astype(jnp.bfloat16)
        for weight in (query_full, key_full, value_full)
    )
    first_col = lax.axis_index("tp") * width_qk
    rate_cols = lax.dynamic_slice_in_dim(decay_up_weight, first_col, width_qk, 1)
    bias_cols = lax.dynamic_slice_in_dim(decay_rate_bias, first_col, width_qk, 0)
    rate_low = jnp.dot(normed, decay_down_weight, preferred_element_type=jnp.float32).astype(
        jnp.bfloat16
    )
    middle, up_full = attend(
        q,
        k,
        v,
        rate_low,
        rate_cols,
        bias_cols,
        decay_increment[0],
        sequence_rows,
        head_norm_gain,
        (up_weight,),
        n,
        n_tp,
    )
    return feed_forward(middle, feedforward_norm_gain, up_full, down_weight, n, n_tp)[None]


def solution(mesh):
    return jax.shard_map(
        functools.partial(per_device, mesh.shape["fs"], mesh.shape["tp"]),
        mesh=mesh,
        in_specs=(
            P(("rep", "fs"), None, None),
            P(),
            P("fs", "tp"),
            P("fs", "tp"),
            P("fs", "tp"),
            P(),
            P(),
            P(),
            P(("rep", "fs"), None, "tp"),
            P(),
            P(),
            P("fs", "tp"),
            P("tp", "fs"),
        ),
        out_specs=P(("rep", "fs"), None, "tp"),
        check_vma=False,
    )
```
